32 devices in a mesh: ep: 8 (over z, x), tp: 4 (over y, core).
Axes of the slice: x: 2, y: 2, z: 4, core: 2. Of those that a mesh axis runs over, the one named last changes fastest.
Arguments:
- mixer_input: bfloat16 [1024, 2048], P('ep'), may hold values from -6 to 6
- mixer_gain: float32 [2048], replicated, may hold values from 0.1 to 1.9
- outer_weight: bfloat16 [2048, 1024], P(None, 'tp'), may hold values from -0.125 to 0.125
- inner_weight: bfloat16 [2048, 1024], P(None, 'tp'), may hold values from -0.125 to 0.125
- value_weight: bfloat16 [2048, 1024], P(None, 'tp'), may hold values from -0.125 to 0.125
- conv_kernel: bfloat16 [3, 1024], P(None, 'tp'), may hold values from -3 to 3
- group_gain: float32 [1024], P('tp'), may hold values from 0.1 to 1.9
- mixer_out_weight: bfloat16 [1024, 2048], P(None, 'tp'), may hold values from -0.1875 to 0.1875
- expert_input: bfloat16 [2048, 2048], P('ep'), may hold values from -6 to 6
- expert_gain: float32 [2048], replicated, may hold values from 0.1 to 1.9
- routes: int32 [2048, 2], P('ep'), may hold values from 0 to 7, all different within a row; in each aligned block of 256 rows (0 to 255, 256 to 511, ...) at most 128 rows name the same one
- route_weight: float32 [2048, 2], P('ep'), may hold values from 0.1 to 1
- expert_gate: bfloat16 [8, 2048, 3584], P('ep', None, 'tp'), may hold values from -0.125 to 0.125
- expert_up: bfloat16 [8, 2048, 3584], P('ep', None, 'tp'), may hold values from -0.125 to 0.125
- expert_down: bfloat16 [8, 3584, 2048], P('ep', None, 'tp'), may hold values from -0.09375 to 0.09375
Outputs:
- mixed_tokens: bfloat16 [1024, 2048], P('ep', 'tp')
- expert_tokens: bfloat16 [2048, 2048], P('ep', 'tp')
The draws below stay inside these ranges and needn't reach their ends.
Inputs may be any that keep to these rules, and one draw needn't show every extreme that they name: `routes`: each row names 2 different experts. Within the rows of one index of ep no expert is named by more than 128 rows, a bound that some block reaches of them.
All inputs are finite; a program needn't handle non-finite values.
Results may differ from the reference program's by a relative error of at most 0.014.
Values may be sent and summed in bfloat16 or wider, within the bound.
A program may use at most 64 MiB of HBM per device.

```python
import math
import jax
import jax.numpy as jnp
import numpy as np
from jax import lax

D = 2048
CONV = 1024
GROUP = 64
FF = 3584
TOP = 2
EXP_ROWS = 256
EXPERTS = 8
CAP = 128
MIX_TOKENS = 1024
EXP_TOKENS = 2048
N_EP = 8


def level_of(rng, extent, cuts, smallest, high):
    loudness = 1.0
    for dim, blocks in cuts:
        draws = jax.random.uniform(jax.random.fold_in(jax.random.fold_in(rng, 6), dim), (blocks,), jnp.float32, smallest / len(cuts), high / len(cuts))
        loudness = loudness * jnp.repeat(jnp.exp(draws), extent[dim] // blocks).reshape((-1,) + (1,) * (len(extent) - 1 - dim))
    return loudness


def assign_block(own_key, own, number, rows, count, top, bound, skew):
    ranking = jax.random.permutation(own_key, count)
    packed, common = load_shares(count, rows * top, bound, skew, True), load_shares(count, rows * top, bound, skew, False)
    places = jnp.arange(count)

    def named(tallies, turn):
        used = int((tallies > 0).sum())
        fixed = max(1, used // 4)
        passed = fixed + (places - fixed + turn * (used - fixed)) % max(1, count - fixed)
        return jnp.zeros((count,), jnp.int32).at[ranking[jnp.where(places < fixed, places, passed)]].set(jnp.asarray(tallies, jnp.int32))

    tallies = jnp.where(number % 4 == 0, named(packed, number // 4), named(common, number - number // 4 - 1))
    mixed = jax.random.permutation(jax.random.fold_in(own, 3), count)
    source_of, taker = mixed[0:count // 2 * 2:2], mixed[1:count // 2 * 2:2]
    room = jnp.minimum(tallies[source_of] - 1, bound - tallies[taker]) // 2
    room = jnp.where((source_of == ranking[0]) | (taker == ranking[0]) | (tallies[taker] == 0), 0, jnp.maximum(room, 0))
    passed = jax.random.randint(jax.random.fold_in(own, 4), (count // 2,), 0, 1 << 20) % (room + 1)
    tallies = tallies.at[source_of].add(-passed).at[taker].add(passed)
    members = jnp.searchsorted(jnp.cumsum(tallies), jnp.arange(rows * top), side="right").astype(jnp.int32)
    table = members.reshape(top, rows).T
    table = table[jax.random.permutation(jax.random.fold_in(own, 1), rows)]
    turn = jax.random.randint(jax.random.fold_in(own, 2), (rows, 1), 0, top)
    return jnp.take_along_axis(table, (jnp.arange(top)[None, :] + turn) % top, axis=1)


def load_shares(count, total, most, skew, full):
    loads = [(1 << 20) // math.isqrt(rank ** skew) + 1 for rank in range(1, count + 1)]
    largest = most if full else min(most, max(-(-total // count), total * loads[0] // sum(loads)))
    least = 1 if total - largest >= count - 1 else 0
    holding, surplus = [largest] + [least] * (count - 1), total - largest - least * (count - 1)
    while surplus > 0:
        movable = [i for i in range(1, count) if holding[i] < largest] or [i for i in range(1, count) if holding[i] < most]
        whole, remaining = sum([loads[i] for i in movable]), surplus
        for i in movable:
            addition = min(most - holding[i], max(1, remaining * loads[i] // whole), surplus)
            holding[i] = holding[i] + addition
            surplus = surplus - addition
    return np.array(holding)


def scatter_about(stream_key, dims, spread, limit, shards=(), kind=jnp.bfloat16):
    values = spread * jax.random.normal(stream_key, dims, jnp.float32)
    if shards:
        values = values * level_of(stream_key, dims, shards, -0.22, 0.18)
    return jnp.clip(values, -limit, limit).astype(kind)


def setup_inputs(seed: int = 0) -> dict:
    splits = jax.random.split(jax.random.key(seed), 16)
    mixer_input = scatter_about(splits[0], (MIX_TOKENS, D), 1.0, 6.0, ((0, 8),))
    mixer_gain = jnp.clip(1.0 + 0.18 * jax.random.normal(splits[1], (D,), jnp.float32), 0.1, 1.9)
    outer_weight = scatter_about(splits[2], (D, CONV), D ** -0.5, 0.125, ((1, 4),))
    inner_weight = scatter_about(splits[3], (D, CONV), D ** -0.5, 0.125, ((1, 4),))
    value_weight = scatter_about(splits[4], (D, CONV), D ** -0.5, 0.125, ((1, 4),))
    conv_kernel = scatter_about(splits[5], (3, CONV), 0.6, 3.0, ((1, 4),))
    group_gain = jnp.clip(1.0 + 0.18 * jax.random.normal(splits[6], (CONV,), jnp.float32), 0.1, 1.9)
    mixer_out_weight = scatter_about(splits[7], (CONV, D), CONV ** -0.5, 0.1875, ((1, 4),))
    expert_input = scatter_about(splits[8], (EXP_TOKENS, D), 1.0, 6.0, ((0, 8),))
    expert_gain = jnp.clip(1.0 + 0.18 * jax.random.normal(splits[9], (D,), jnp.float32), 0.1, 1.9)
    routes_keys = jax.random.split(jax.random.fold_in(splits[10], 1), EXP_TOKENS // EXP_ROWS)
    routes_turns = jax.random.permutation(jax.random.fold_in(splits[10], 3), EXP_TOKENS // EXP_ROWS)
    routes = jax.vmap(lambda own, number: assign_block(jax.random.fold_in(splits[10], 2), own, number, EXP_ROWS, EXPERTS, TOP, CAP, 2))(routes_keys, routes_turns).reshape((EXP_TOKENS, TOP))
    route_weight = jnp.clip(0.1 + 0.9 * jax.random.uniform(splits[11], (EXP_TOKENS, TOP), jnp.float32) ** level_of(splits[11], (EXP_TOKENS, TOP), ((0, 8),), -0.2, 0.2), 0.1, 1.0)
    expert_gate = scatter_about(splits[12], (EXPERTS, D, FF), D ** -0.5, 0.125, ((0, 8), (2, 4)))
    expert_up = scatter_about(splits[13], (EXPERTS, D, FF), D ** -0.5, 0.125, ((0, 8), (2, 4)))
    expert_down = scatter_about(splits[14], (EXPERTS, FF, D), FF ** -0.5, 0.09375, ((0, 8), (2, 4)))
    return dict(mixer_input=mixer_input, mixer_gain=mixer_gain, outer_weight=outer_weight, inner_weight=inner_weight, value_weight=value_weight, conv_kernel=conv_kernel, group_gain=group_gain, mixer_out_weight=mixer_out_weight, expert_input=expert_input, expert_gain=expert_gain, routes=routes, route_weight=route_weight, expert_gate=expert_gate, expert_up=expert_up, expert_down=expert_down)


EPS = 1e-06

def rms_scale(values, gain):
    floats = values.astype(jnp.float32)
    scale = lax.rsqrt(lax.optimization_barrier(jnp.mean(floats * floats, axis=-1, keepdims=True)) + EPS)
    return floats * scale * gain.astype(jnp.float32)

def run_expert(operands):
    rows, gate_part, up_part, down_part = operands
    gate = jnp.dot(rows, gate_part, preferred_element_type=jnp.float32)
    up_value = jnp.dot(rows, up_part, preferred_element_type=jnp.float32)
    hidden = (jax.nn.silu(gate) * up_value).astype(jnp.bfloat16)
    return jnp.dot(hidden, down_part, preferred_element_type=jnp.float32).astype(jnp.bfloat16)

def reference(mixer_input, mixer_gain, outer_weight, inner_weight, value_weight, conv_kernel, group_gain, mixer_out_weight, expert_input, expert_gain, routes, route_weight, expert_gate, expert_up, expert_down):
    count = mixer_input.shape[0]
    normed_a = rms_scale(mixer_input, mixer_gain).astype(jnp.bfloat16)
    outer = jnp.dot(normed_a, outer_weight, preferred_element_type=jnp.float32).astype(jnp.bfloat16)
    inner = jnp.dot(normed_a, inner_weight, preferred_element_type=jnp.float32).astype(jnp.bfloat16)
    values = jnp.dot(normed_a, value_weight, preferred_element_type=jnp.float32).astype(jnp.bfloat16)
    product = inner.astype(jnp.float32) * values.astype(jnp.float32)
    padded = jnp.pad(product, ((2, 0), (0, 0)))
    kernel = conv_kernel.astype(jnp.float32)
    conv_sum = kernel[0] * padded[0:count] + kernel[1] * padded[1:count + 1] + kernel[2] * padded[2:count + 2]
    gated = outer.astype(jnp.float32) * conv_sum
    grouped = gated.reshape(count, CONV // GROUP, GROUP)
    grouped = rms_scale(grouped, group_gain.reshape(CONV // GROUP, GROUP))
    grouped = grouped.reshape(count, CONV).astype(jnp.bfloat16)
    mixed_tokens = jnp.dot(grouped, mixer_out_weight, preferred_element_type=jnp.float32).astype(jnp.bfloat16)
    normed_b = rms_scale(expert_input, expert_gain).astype(jnp.bfloat16)
    picks = routes.reshape(N_EP, EXP_ROWS * TOP).astype(jnp.int32)
    onehot = (picks[:, :, None] == jnp.arange(EXPERTS, dtype=jnp.int32)[None, None, :]).astype(jnp.int32)
    earlier = jnp.cumsum(onehot, axis=1) - onehot
    rank = lax.optimization_barrier(jnp.sum(earlier * onehot, axis=2)).astype(jnp.int32)
    slot = (picks * CAP + rank).astype(jnp.int32)
    token = (jnp.arange(EXP_ROWS * TOP, dtype=jnp.int32) // TOP).astype(jnp.int32)
    source = jnp.arange(N_EP, dtype=jnp.int32)[:, None]
    table = jnp.zeros((N_EP, EXPERTS * CAP), jnp.int32).at[source, slot].set(token[None, :] + 1)
    valid = table > 0
    row_index = (source * EXP_ROWS + jnp.maximum(table - 1, 0)).astype(jnp.int32)
    buffer = jnp.where(valid[..., None], jnp.take(normed_b, row_index, axis=0), 0).astype(jnp.bfloat16)
    per_expert = buffer.reshape(N_EP, EXPERTS, CAP, D).transpose(1, 0, 2, 3).reshape(EXPERTS, N_EP * CAP, D)
    outputs = lax.map(run_expert, (per_expert, expert_gate, expert_up, expert_down))
    flat_out = outputs.reshape(EXPERTS * N_EP * CAP, D)
    position = (picks * (N_EP * CAP) + source * CAP + rank).astype(jnp.int32)
    chosen = jnp.take(flat_out, position.reshape(-1), axis=0).astype(jnp.float32).reshape(N_EP * EXP_ROWS, TOP, D)
    weighted = lax.optimization_barrier(jnp.sum(chosen * route_weight.astype(jnp.float32)[..., None], axis=1))
    expert_tokens = weighted.astype(jnp.bfloat16)
    return (mixed_tokens, expert_tokens)
```

```python
import functools

import jax
import jax.numpy as jnp
from jax import lax
from jax.experimental import pallas as pl
from jax.experimental.pallas import tpu as pltpu
from jax.sharding import PartitionSpec as P

GROUP = 64


EPS = 1e-06


def from_behind(block, axis, distance):
    devices = range(lax.axis_size(axis))
    route = [(i - distance, i) for i in devices if i - distance in devices]
    return lax.ppermute(block, axis, route)


def rms_scale(values, gain):
    floats = values.astype(jnp.float32)
    scale = lax.rsqrt(jnp.mean(floats * floats, axis=-1, keepdims=True) + EPS)
    return floats * scale * gain


F32 = jnp.float32
BF16 = jnp.bfloat16


def flip(index, offset, count):
    out = index
    bit = 1
    while bit < count:
        out = out + bit * ((offset // bit) % 2) * (1 - 2 * ((index // bit) % 2))
        bit *= 2
    return out


def matmul(a, b):
    return jnp.dot(a, b, preferred_element_type=F32)


def doubled(n_ep):
    return [*range(n_ep - 1, n_ep)]


def send_order(n_ep):
    half = n_ep // 2
    quarter = half // 2
    far = [half + i + j * quarter for i in range(quarter) for j in range(2)]
    return [1, *far[:2]], far[2:], [*range(half - 1, 1, -1)]


def turns(n_ep):
    half = n_ep // 2
    return [0, 1, *range(half, n_ep), *range(half - 1, 1, -1)]


def schedule(n_ep):
    half = n_ep // 2
    far = [m for m in range(half, n_ep) if m not in doubled(n_ep)]
    order = turns(n_ep)
    steps, crossing = [], [("hidden", 0)]

    def take(item):
        while item in crossing:
            steps.append(crossing.pop(0))

    def send(name, m, item):
        steps.append((name, m))
        crossing.append((item, m))

    def arrive(m):
        steps.append(("near" if m < half else "both", m))

    arrive(1)
    send("pass_far", far[0], "far")
    for k in range(1, n_ep):
        m = order[k]
        take(("far", m))
        if 2 <= k <= len(far):
            send("pass_far", far[k - 1], "far")
        steps += [("ready", m)]
        if k + 1 == n_ep:
            steps += [("contract", order[k - 2])]
        send("expand", m, "hidden")
        if k + 1 < n_ep and order[k + 1] not in far:
            arrive(order[k + 1])
        if k == 5:
            send("mix_convolve", 0, "mix")
        if 2 <= k < n_ep - 1:
            steps += [("contract", order[k - 2])]
        take(("hidden", order[k - 1]))
    steps += [("contract", order[-2]), ("gather", 0), ("gather", 1)]
    steps += [("last", 0), ("last", 1)]
    return steps + [("gather", m) for m in order[2:]]


def experts_kernel(
    n_ep,
    mix_hbm,
    mix_gain_hbm,
    kernel_hbm,
    group_gain_hbm,
    x_hbm,
    gain_hbm,
    routes_hbm,
    weight_hbm,
    outer_hbm,
    inner_hbm,
    value_hbm,
    mix_out_hbm,
    gate_hbm,
    up_hbm,
    down_hbm,
    mix_o_ref,
    o_ref,
    mix_ref,
    mix_gain_ref,
    kernel_ref,
    group_gain_ref,
    x_ref,
    gain_ref,
    routes_ref,
    weight_ref,
    nb,
    xs,
    xb,
    wgu,
    wd,
    hb,
    rs,
    ret,
    whi,
    wlo,
    total,
    na,
    wmix,
    wmo,
    padded,
    outer,
    grouped,
    i_sem,
    w_sem,
    s_sem,
    r_sem,
):
    ep = lax.axis_index("ep")
    tp = lax.axis_index("tp")
    y, core = tp // 2, tp % 2
    partner = {"tp": y * 2 + 1 - core}
    across = {"tp": (1 - y) * 2 + core}
    over_tp = (1 - y) * 2 + core
    half = n_ep // 2
    quarter = half // 2
    inner = (ep // half + ep // quarter) % 2
    rows = x_ref.shape[0]
    cap = xb.shape[2]
    span = xb.shape[3]
    tiles, depth, pair = wgu.shape
    tile = pair // 2
    part = hb.shape[3]
    out_cols = wd.shape[1]

    barrier = pltpu.get_barrier_semaphore()
    peers = [{"ep": flip(ep, m, n_ep)} for m in range(1, n_ep)] + [partner, across]
    for peer in peers:
        pl.semaphore_signal(barrier, inc=1, device_id=peer, device_id_type=pl.DeviceIdType.MESH)

    chunk = 64
    chunks = rows // chunk
    fetch_x = [
        pltpu.make_async_copy(
            x_hbm.at[pl.ds(i * chunk, chunk)], x_ref.at[pl.ds(i * chunk, chunk)], i_sem.at[i]
        )
        for i in range(chunks)
    ]
    fetch_small = [
        pltpu.make_async_copy(src, dst, i_sem.at[chunks + i])
        for i, (src, dst) in enumerate(
            (
                (gain_hbm, gain_ref),
                (routes_hbm, routes_ref),
                (weight_hbm, weight_ref),
                (mix_gain_hbm, mix_gain_ref),
                (kernel_hbm, kernel_ref),
                (group_gain_hbm, group_gain_ref),
                (mix_hbm, mix_ref),
            )
        )
    ]
    fetches = []
    for j in range(tiles):
        cols = pl.ds(j * tile, tile)
        fetches.append(
            (
                pltpu.make_async_copy(
                    gate_hbm.at[0, :, cols], wgu.at[j, :, pl.ds(0, tile)], w_sem.at[2 * j]
                ),
                pltpu.make_async_copy(
                    up_hbm.at[0, :, cols], wgu.at[j, :, pl.ds(tile, tile)], w_sem.at[2 * j + 1]
                ),
            )
        )
    fetch_down = pltpu.make_async_copy(down_hbm.at[0], wd, w_sem.at[2 * tiles])
    fetch_mix = [
        pltpu.make_async_copy(src, wmix.at[i], w_sem.at[2 * tiles + 1 + i])
        for i, src in enumerate((outer_hbm, inner_hbm, value_hbm))
    ]
    fetch_mix_out = pltpu.make_async_copy(mix_out_hbm, wmo, w_sem.at[2 * tiles + 4])
    fetch_small[0].start()
    for copy in fetch_x:
        copy.start()
    for copy in fetch_small[1:-1]:
        copy.start()
    for a, b in fetches:
        a.start()
        b.start()

    step_rows = 32

    def normalize(src, gain, dst, start, count):
        def norm(i, carry):
            at = pl.ds(pl.multiple_of(i * step_rows, step_rows), step_rows)
            v = src[at, :].astype(F32)
            scale = lax.rsqrt(jnp.mean(v * v, axis=-1, keepdims=True) + EPS)
            dst[at, :] = (v * scale * gain[...]).astype(BF16)
            return carry

        lax.fori_loop(start // step_rows, (start + count) // step_rows, norm, 0)

    fetch_small[0].wait()
    for i in range(chunks):
        fetch_x[i].wait()
        normalize(x_ref, gain_ref, nb, i * chunk, chunk)
    fetch_small[-1].start()
    for copy in fetch_mix:
        copy.start()
    fetch_down.start()
    fetch_mix_out.start()

    fetch_small[1].wait()
    first = routes_ref[0:1, :]
    second = routes_ref[1:2, :]
    masks = []
    level = lax.broadcasted_iota(jnp.int32, (n_ep, rows), 0)
    stacked = jnp.zeros((n_ep, rows), F32)
    for m in range(n_ep):
        e = flip(ep, m, n_ep)
        mask = jnp.where((first == e) | (second == e), 1.0, 0.0)
        masks.append(mask)
        stacked = jnp.where(level == m, mask, stacked)
    upper = lax.broadcasted_iota(jnp.int32, (rows, rows), 0) < lax.broadcasted_iota(
        jnp.int32, (rows, rows), 1
    )
    ranks = matmul(stacked.astype(BF16), jnp.where(upper, 1.0, 0.0).astype(BF16))
    slots = lax.broadcasted_iota(jnp.int32, (cap, rows), 0).astype(F32)

    def place(m):
        return jnp.where((slots == ranks[m : m + 1, :]) & (masks[m] > 0.5), 1.0, 0.0)

    def remote(src, dst, kind, m, device):
        return pltpu.make_async_remote_copy(
            src_ref=src,
            dst_ref=dst,
            send_sem=s_sem.at[kind, m],
            recv_sem=r_sem.at[kind, m],
            device_id=device,
            device_id_type=pl.DeviceIdType.MESH,
        )

    def label(turn):
        if turn < half:
            return turn
        r = turn - half
        return turn + (1 - inner) * (quarter - 2 * quarter * (r // quarter))

    def source_of(m):
        return {"ep": flip(ep, m, n_ep)}

    mine2 = pl.ds(core * 2, 2)

    def near_rows(m):
        return remote(xs.at[m], xb.at[m, mine2], 0, m, source_of(m))

    def near_partner(m):
        return remote(xb.at[m, mine2], xb.at[m, mine2], 1, m, partner)

    def far_rows(m):
        return remote(xs.at[m, 0], xb.at[m, tp], 0, m, source_of(m))

    def far_rows_over(m):
        return remote(xs.at[m, 1], xb.at[m, over_tp], 12, m, source_of(m))

    def far_partner(m):
        return remote(xb.at[m, tp], xb.at[m, tp], 1, m, partner)

    def far_across(m):
        return remote(xb.at[m, tp], xb.at[m, tp], 2, m, across)

    def far_relay(m):
        return remote(xb.at[m, over_tp], xb.at[m, over_tp], 3, m, partner)

    mid = (tiles + 1) // 2
    pieces = [(0, mid), (mid, tiles)]

    final = turns(n_ep)[-1]
    half_cap = cap // 2

    def final_turn(m):
        return isinstance(m, int) and m == final

    def hidden_piece(m, where, p):
        if final_turn(m):
            return hb.at[m, where, pl.ds(p * half_cap, half_cap)]
        lo, hi = pieces[p]
        return hb.at[m, where, :, pl.ds(lo * tile, (hi - lo) * tile)]

    def hid_partner(m, p):
        return remote(hidden_piece(m, tp, p), hidden_piece(m, tp, p), 4 + 5 * p, m, partner)

    def hid_across(m, p):
        return remote(hidden_piece(m, tp, p), hidden_piece(m, tp, p), 5 + 5 * p, m, across)

    def hid_relay(m, p):
        return remote(hidden_piece(m, over_tp, p), hidden_piece(m, over_tp, p), 6 + 5 * p, m, partner)

    def back(m):
        return remote(rs.at[m], ret.at[m], 7, m, source_of(m))

    def back_final(p):
        at = pl.ds(p * half_cap, half_cap)
        return remote(rs.at[final, at], ret.at[final, at], 7 + 6 * p, final, source_of(final))

    def dispatch(m):
        chosen = place(m).astype(BF16)
        if m < half:
            for k in range(2):
                at = pl.ds(pl.multiple_of((core * 2 + k) * span, span), span)
                xs[m, k] = matmul(chosen, nb[:, at]).astype(BF16)
        else:
            at = pl.ds(pl.multiple_of(tp * span, span), span)
            xs[m, 0] = matmul(chosen, nb[:, at]).astype(BF16)
            if m % quarter + half + quarter in doubled(n_ep):
                at = pl.ds(pl.multiple_of(over_tp * span, span), span)
                xs[m, 1] = matmul(chosen, nb[:, at]).astype(BF16)
        if m == 1:
            pl.semaphore_wait(barrier, len(peers))
        if m < half:
            near_rows(m).start()
        else:
            far_rows(m).start()
            if m % quarter + half + quarter in doubled(n_ep):

                @pl.when(inner == 1)
                def _():
                    far_rows_over(m).start()

    def expand(turn):
        m = label(turn)

        def body(j, carry):
            if turn == 0:
                pltpu.make_async_copy(
                    gate_hbm.at[0, :, pl.ds(0, tile)], wgu.at[j, :, pl.ds(0, tile)], w_sem.at[2 * j]
                ).wait()
                pltpu.make_async_copy(
                    up_hbm.at[0, :, pl.ds(0, tile)],
                    wgu.at[j, :, pl.ds(tile, tile)],
                    w_sem.at[2 * j + 1],
                ).wait()
            acc = matmul(xb[m, 0], wgu[j, 0:span, :])
            for k in range(1, depth // span):
                acc = acc + matmul(xb[m, k], wgu[j, k * span : (k + 1) * span, :])
            g, u = acc[:, :tile], acc[:, tile:]
            hidden = g / (1.0 + jnp.exp(-g)) * u
            hb[m, tp, :, pl.ds(pl.multiple_of(j * tile, tile), tile)] = hidden.astype(BF16)
            return carry

        for p, (lo, hi) in enumerate(pieces):
            lax.fori_loop(lo, hi, body, 0)
            if not final_turn(m):
                hid_across(m, p).start()
                hid_partner(m, p).start()
        if final_turn(m):
            for p in range(2):
                hid_across(m, p).start()
                hid_partner(m, p).start()

    block = 256

    def contract(turn):
        m = label(turn)
        for p in range(len(pieces)):
            hid_partner(m, p).wait_recv()
            hid_relay(m, p).wait_recv()
        for n in range(out_cols // block):
            cols = slice(n * block, (n + 1) * block)
            acc = matmul(hb[m, 0], wd[0:part, cols])
            for k in range(1, hb.shape[1]):
                acc = acc + matmul(hb[m, k], wd[k * part : (k + 1) * part, cols])
            if turn == 0:
                ret[0, :, cols] = acc.astype(BF16)
            else:
                rs[m, :, cols] = acc.astype(BF16)
        if turn:
            back(m).start()

    def last(p):
        if p == 0:
            hid_across(final, 0).wait_recv()
            hid_relay(final, 0).start()
        hid_partner(final, p).wait_recv()
        hid_relay(final, p).wait_recv()
        at = slice(p * half_cap, (p + 1) * half_cap)
        for n in range(out_cols // block):
            cols = slice(n * block, (n + 1) * block)
            acc = matmul(hb[final, 0, at], wd[0:part, cols])
            for k in range(1, hb.shape[1]):
                acc = acc + matmul(hb[final, k, at], wd[k * part : (k + 1) * part, cols])
            rs[final, at, cols] = acc.astype(BF16)
        back_final(p).start()
        if p == 0:
            hid_across(final, 1).wait_recv()
            hid_relay(final, 1).start()

    def pass_hidden(turn):
        for p in range(len(pieces)):
            hid_across(label(turn), p).wait_recv()
            hid_relay(label(turn), p).start()

    def pass_near(m):
        near_rows(m).wait_recv()
        near_partner(m).start()

    def pass_both(turn):
        m = label(turn)
        far_rows(m).wait_recv()
        far_partner(m).start()
        far_rows_over(m).wait_recv()
        far_relay(m).start()

    def pass_far(turn):
        m = label(turn)
        far_rows(m).wait_recv()
        far_across(m).start()
        far_partner(m).start()

    def pass_relay(turn):
        m = label(turn)
        far_across(m).wait_recv()
        far_relay(m).start()

    def ready(turn):
        m = label(turn)
        if turn < half:
            near_partner(m).wait_recv()
        else:
            far_partner(m).wait_recv()
            far_relay(m).wait_recv()

    mix_rows, channels = outer.shape
    halo = padded.shape[0] - mix_rows
    ahead = {"ep": lax.rem(ep + 1, n_ep)}
    send_halo = remote(padded.at[pl.ds(mix_rows, halo)], padded.at[pl.ds(0, halo)], 8, 0, ahead)
    mix_partner = remote(grouped.at[tp], grouped.at[tp], 8, 1, partner)
    mix_across = remote(grouped.at[tp], grouped.at[tp], 8, 2, across)
    mix_relay = remote(grouped.at[over_tp], grouped.at[over_tp], 8, 3, partner)

    def mix_project():
        for copy in fetch_small[3:]:
            copy.wait()
        normalize(mix_ref, mix_gain_ref, na, 0, mix_rows)
        for copy in fetch_mix:
            copy.wait()
        outer[...] = matmul(na[...], wmix[0]).astype(BF16)
        inner = matmul(na[...], wmix[1]).astype(BF16).astype(F32)
        padded[pl.ds(halo, mix_rows), :] = inner * matmul(na[...], wmix[2]).astype(BF16).astype(F32)

        @pl.when(ep < n_ep - 1)
        def _():
            send_halo.start()

        @pl.when(ep == 0)
        def _():
            padded[pl.ds(0, halo), :] = jnp.zeros((halo, channels), F32)

    def mix_convolve(_):
        @pl.when(ep > 0)
        def _():
            send_halo.wait_recv()

        taps = kernel_ref[...].astype(F32)
        conv = taps[2:3, :] * padded[pl.ds(halo, mix_rows), :]
        for back_by in (1, 2):
            conv = conv + taps[2 - back_by : 3 - back_by, :] * padded[pl.ds(halo - back_by, mix_rows), :]
        gated = outer[...].astype(F32) * conv
        squares = gated * gated
        group = lax.broadcasted_iota(jnp.int32, (mix_rows, channels), 1) // GROUP
        scale = jnp.zeros_like(gated)
        for i in range(channels // GROUP):
            mean = jnp.sum(jnp.where(group == i, squares, 0.0), axis=-1, keepdims=True) / GROUP
            scale = jnp.where(group == i, lax.rsqrt(mean + EPS), scale)
        grouped[tp] = (gated * scale * group_gain_ref[...]).astype(BF16)
        mix_across.start()
        mix_partner.start()

    def mix_pass(_):
        mix_across.wait_recv()
        mix_relay.start()

    def mix_contract():
        fetch_mix_out.wait()
        mix_partner.wait_recv()
        mix_relay.wait_recv()
        acc = matmul(grouped[0], wmo[0:channels, :])
        for k in range(1, grouped.shape[0]):
            acc = acc + matmul(grouped[k], wmo[k * channels : (k + 1) * channels, :])
        mix_o_ref[...] = acc.astype(BF16)

    def build_weights():
        fetch_small[2].wait()
        for m in range(n_ep):
            picked = jnp.where(first == flip(ep, m, n_ep), weight_ref[0:1, :], weight_ref[1:2, :])
            scaled = (place(m) * picked).T
            high = scaled.astype(BF16)
            whi[:, m * cap : (m + 1) * cap] = high
            wlo[:, m * cap : (m + 1) * cap] = (scaled - high.astype(F32)).astype(BF16)

    def gather(turn):
        m = label(turn)
        if turn == final:
            back_final(0).wait_recv()
            back_final(1).wait_recv()
        elif turn:
            back(m).wait_recv()
        else:
            mix_contract()
        cols = pl.ds(m * cap if turn < half else pl.multiple_of(m * cap, cap), cap)
        high = matmul(whi[:, cols], ret[m])
        low = matmul(wlo[:, cols], ret[m])
        if turn == 0:
            total[...] = high + low
        else:
            total[...] += high + low

    first_sends, later_sends, last_sends = send_order(n_ep)
    for m in first_sends:
        dispatch(m)
    chosen = place(0).astype(BF16)
    for k in range(depth // span):
        xb[0, k] = matmul(chosen, nb[:, k * span : (k + 1) * span]).astype(BF16)
    expand(0)
    for m in later_sends:
        dispatch(m)
    mix_project()
    build_weights()
    for m in last_sends:
        dispatch(m)
    fetch_down.wait()
    actions = dict(
        last=last, near=pass_near, both=pass_both, pass_far=pass_far, far=pass_relay, ready=ready, expand=expand,
        hidden=pass_hidden, contract=contract, mix_convolve=mix_convolve, mix=mix_pass,
        gather=gather,
    )
    for step, m in schedule(n_ep):
        actions[step](m)
    o_ref[...] = total[...].astype(BF16)

    @pl.when(ep < n_ep - 1)
    def _():
        send_halo.wait_send()

    for copy in (mix_partner, mix_across, mix_relay):
        copy.wait_send()
    for turn in range(n_ep):
        m = label(turn)
        for p in range(len(pieces)):
            for copy in (hid_partner(m, p), hid_across(m, p), hid_relay(m, p)):
                copy.wait_send()
        if turn == final:
            back_final(0).wait_send()
            back_final(1).wait_send()
        elif turn:
            back(m).wait_send()
        if 0 < turn < half:
            near_rows(m).wait_send()
            near_partner(m).wait_send()
        if turn >= half:
            far_rows(m).wait_send()
            far_partner(m).wait_send()
            far_relay(m).wait_send()
            if turn not in doubled(n_ep):
                far_across(m).wait_send()
            if turn % quarter + half + quarter in doubled(n_ep):

                @pl.when(inner == 1)
                def _():
                    far_rows_over(m).wait_send()


def fused(
    mixer_input,
    mixer_gain,
    outer_weight,
    inner_weight,
    value_weight,
    conv_kernel,
    group_gain,
    mixer_out_weight,
    expert_input,
    expert_gain,
    routes,
    route_weight,
    expert_gate,
    expert_up,
    expert_down,
):
    n_ep, n_tp = lax.axis_size("ep"), lax.axis_size("tp")
    rows, width = expert_input.shape
    mix_rows = mixer_input.shape[0]
    channels = outer_weight.shape[1]
    cap = 2 * routes.shape[1] * rows // n_ep
    span = width // n_tp
    part = expert_gate.shape[2]
    tile = 128
    tiles = part // tile
    full, out_cols = expert_down.shape[1:]
    mix_cols = mixer_out_weight.shape[1]
    vmem = pl.BlockSpec(memory_space=pltpu.VMEM)
    hbm = pl.BlockSpec(memory_space=pl.ANY)
    operands = (
        mixer_input,
        mixer_gain.reshape(1, -1),
        conv_kernel,
        group_gain.reshape(1, -1),
        expert_input,
        expert_gain.reshape(1, -1),
        routes.T,
        route_weight.T,
        outer_weight,
        inner_weight,
        value_weight,
        mixer_out_weight,
        expert_gate,
        expert_up,
        expert_down,
    )
    return pl.pallas_call(
        functools.partial(experts_kernel, n_ep),
        out_shape=(
            pltpu.VMEM((mix_rows, mix_cols), BF16),
            pltpu.VMEM((rows, out_cols), BF16),
        ),
        in_specs=[hbm] * len(operands),
        out_specs=(vmem, vmem),
        scratch_shapes=[
            *(pltpu.VMEM(v.shape, v.dtype) for v in operands[:8]),
            pltpu.VMEM((rows, width), BF16),
            pltpu.VMEM((n_ep, 2, cap, span), BF16),
            pltpu.VMEM((n_ep, n_tp, cap, span), BF16),
            pltpu.VMEM((tiles, width, 2 * tile), BF16),
            pltpu.VMEM((full, out_cols), BF16),
            pltpu.VMEM((n_ep, n_tp, cap, part), BF16),
            pltpu.VMEM((n_ep, cap, out_cols), BF16),
            pltpu.VMEM((n_ep, cap, out_cols), BF16),
            pltpu.VMEM((rows, n_ep * cap), BF16),
            pltpu.VMEM((rows, n_ep * cap), BF16),
            pltpu.VMEM((rows, out_cols), F32),
            pltpu.VMEM((mix_rows, width), BF16),
            pltpu.VMEM((3, width, channels), BF16),
            pltpu.VMEM((channels * n_tp, mix_cols), BF16),
            pltpu.VMEM((8 + mix_rows, channels), F32),
            pltpu.VMEM((mix_rows, channels), BF16),
            pltpu.VMEM((n_tp, mix_rows, channels), BF16),
            pltpu.SemaphoreType.DMA((rows // 64 + 7,)),
            pltpu.SemaphoreType.DMA((2 * tiles + 5,)),
            pltpu.SemaphoreType.DMA((14, n_ep)),
            pltpu.SemaphoreType.DMA((14, n_ep)),
        ],
        compiler_params=pltpu.CompilerParams(
            collective_id=0, has_side_effects=True, vmem_limit_bytes=60 * 1024 * 1024
        ),
        name="layer",
    )(*operands)


def fits(n_ep, n_tp, routes, expert_gate):
    return (
        n_tp == 4
        and n_ep >= 8
        and n_ep & (n_ep - 1) == 0
        and routes.shape[1] == 2
        and expert_gate.shape[0] == 1
        and expert_gate.shape[2] % 128 == 0
        and routes.shape[0] % 64 == 0
    )


def mixer_xla(
    mixer_input,
    mixer_gain,
    outer_weight,
    inner_weight,
    value_weight,
    conv_kernel,
    group_gain,
    mixer_out_weight,
):
    mix_count = mixer_input.shape[0]
    normed_a = rms_scale(mixer_input, mixer_gain).astype(jnp.bfloat16)
    outer = jnp.dot(normed_a, outer_weight, preferred_element_type=jnp.float32).astype(jnp.bfloat16)
    inner = jnp.dot(normed_a, inner_weight, preferred_element_type=jnp.float32).astype(jnp.bfloat16)
    values = jnp.dot(normed_a, value_weight, preferred_element_type=jnp.float32).astype(
        jnp.bfloat16
    )
    product = inner.astype(jnp.float32) * values.astype(jnp.float32)
    earlier_rows = from_behind(product[mix_count - 2 :], "ep", 1)
    padded = jnp.concatenate([earlier_rows, product], axis=0)
    kernel = conv_kernel.astype(jnp.float32)
    conv_sum = (
        kernel[0] * padded[0:mix_count]
        + kernel[1] * padded[1 : mix_count + 1]
        + kernel[2] * padded[2 : mix_count + 2]
    )
    gated = outer.astype(jnp.float32) * conv_sum
    grouped = gated.reshape(mix_count, -1, GROUP)
    grouped = rms_scale(grouped, group_gain.reshape(-1, GROUP))
    grouped = grouped.reshape(mix_count, -1).astype(jnp.bfloat16)
    weight_rows = mixer_out_weight
    mixed_tokens = jnp.dot(
        lax.all_gather(grouped, "tp", axis=1, tiled=True),
        weight_rows,
        preferred_element_type=jnp.float32,
    ).astype(jnp.bfloat16)
    return mixed_tokens


def experts_xla(
    expert_input,
    expert_gain,
    routes,
    route_weight,
    expert_gate,
    expert_up,
    expert_down,
):
    exp_count, picks_each = routes.shape
    width = expert_input.shape[1]
    experts = expert_gate.shape[0] * lax.axis_size("ep")
    capacity = 2 * picks_each * exp_count // experts
    normed_b = rms_scale(expert_input, expert_gain).astype(jnp.bfloat16)
    picks = routes.reshape(-1)
    onehot = (picks[:, None] == jnp.arange(experts, dtype=jnp.int32)[None, :]).astype(jnp.int32)
    rank = jnp.sum((jnp.cumsum(onehot, axis=0) - onehot) * onehot, axis=1)
    slot = picks * capacity + rank
    token = jnp.arange(exp_count * picks_each, dtype=jnp.int32) // picks_each
    table = jnp.zeros((experts * capacity,), jnp.int32).at[slot].set(token + 1)
    valid = table > 0
    gathered_rows = jnp.take(normed_b, jnp.maximum(table - 1, 0), axis=0)
    buffer = jnp.where(valid[:, None], gathered_rows, 0).reshape(experts, capacity, width)
    gate_weight = expert_gate[0]
    up_weight = expert_up[0]
    down_weight = expert_down[0]
    out_cols = down_weight.shape[1]
    span = width // lax.axis_size("tp")
    outgoing = lax.dynamic_slice_in_dim(buffer, lax.axis_index("tp") * span, span, 2)
    received = lax.all_to_all(outgoing, "ep", split_axis=0, concat_axis=0, tiled=True)
    sources = received.shape[0]
    count = received.shape[1]
    piece = lax.all_gather(received, "tp", axis=2, tiled=True)
    span = piece.shape[2]
    flat_piece = piece.reshape(sources * count, span)
    gate = jnp.dot(flat_piece, gate_weight, preferred_element_type=jnp.float32)
    up_value = jnp.dot(flat_piece, up_weight, preferred_element_type=jnp.float32)
    hidden = (jax.nn.silu(gate) * up_value).astype(jnp.bfloat16)
    weight_rows = down_weight
    results = jnp.dot(
        lax.all_gather(hidden, "tp", axis=1, tiled=True),
        weight_rows,
        preferred_element_type=jnp.float32,
    ).astype(jnp.bfloat16)
    returned = lax.all_to_all(
        results.reshape(sources, count, out_cols), "ep", split_axis=0, concat_axis=0, tiled=True
    )
    flat_returned = returned.reshape(experts * capacity, out_cols)
    chosen = (
        jnp.take(flat_returned, slot, axis=0)
        .astype(jnp.float32)
        .reshape(exp_count, picks_each, out_cols)
    )
    weighted = jnp.sum(chosen * route_weight[..., None], axis=1)
    expert_tokens = weighted.astype(jnp.bfloat16)
    return expert_tokens


def per_device(*args):
    n_ep, n_tp = lax.axis_size("ep"), lax.axis_size("tp")
    if fits(n_ep, n_tp, args[10], args[12]):
        return fused(*args)
    return mixer_xla(*args[:8]), experts_xla(*args[8:])


def solution(mesh):
    placed = (
        P("ep", None),
        P(),
        P(None, "tp"),
        P(None, "tp"),
        P(None, "tp"),
        P(None, "tp"),
        P("tp"),
        P(None, "tp"),
        P("ep", None),
        P(),
        P("ep", None),
        P("ep", None),
        P("ep", None, "tp"),
        P("ep", None, "tp"),
        P("ep", None, "tp"),
    )
    return jax.shard_map(
        per_device,
        mesh=mesh,
        in_specs=placed,
        out_specs=(P("ep", "tp"), P("ep", "tp")),
        check_vma=False,
    )
```

```python
import functools

import jax
import jax.numpy as jnp
from jax import lax
from jax.experimental import pallas as pl
from jax.experimental.pallas import tpu as pltpu
from jax.sharding import PartitionSpec as P

GROUP = 64


EPS = 1e-06


def from_behind(block, axis, distance):
    devices = range(lax.axis_size(axis))
    route = [(i - distance, i) for i in devices if i - distance in devices]
    return lax.ppermute(block, axis, route)


def rms_scale(values, gain):
    floats = values.astype(jnp.float32)
    scale = lax.rsqrt(jnp.mean(floats * floats, axis=-1, keepdims=True) + EPS)
    return floats * scale * gain


F32 = jnp.float32
BF16 = jnp.bfloat16


def flip(index, offset, count):
    out = index
    bit = 1
    while bit < count:
        out = out + bit * ((offset // bit) % 2) * (1 - 2 * ((index // bit) % 2))
        bit *= 2
    return out


def matmul(a, b):
    return jnp.dot(a, b, preferred_element_type=F32)


def doubled(n_ep):
    return [*range(n_ep - 1, n_ep)]


def send_order(n_ep):
    half = n_ep // 2
    quarter = half // 2
    far = [half + i + j * quarter for i in range(quarter) for j in range(2)]
    return [1, *far[:2]], far[2:], [*range(half - 1, 1, -1)]


def turns(n_ep):
    half = n_ep // 2
    return [0, 1, *range(half, n_ep), *range(half - 1, 1, -1)]


def schedule(n_ep):
    half = n_ep // 2
    far = [m for m in range(half, n_ep) if m not in doubled(n_ep)]
    order = turns(n_ep)
    steps, crossing = [], [("hidden", 0)]

    def take(item):
        while item in crossing:
            steps.append(crossing.pop(0))

    def send(name, m, item):
        steps.append((name, m))
        crossing.append((item, m))

    def arrive(m):
        steps.append(("near" if m < half else "both", m))

    arrive(1)
    send("pass_far", far[0], "far")
    for k in range(1, n_ep):
        m = order[k]
        take(("far", m))
        if 2 <= k <= len(far):
            send("pass_far", far[k - 1], "far")
        steps += [("ready", m)]
        if k + 1 == n_ep:
            steps += [("contract", order[k - 2])]
        send("expand", m, "hidden")
        if k + 1 < n_ep and order[k + 1] not in far:
            arrive(order[k + 1])
        if k + 1 == n_ep:
            steps += [("mix_convolve", 0)]
        if 2 <= k < n_ep - 1:
            steps += [("contract", order[k - 2])]
        take(("hidden", order[k - 1]))
    steps += [("contract", order[-2]), ("gather", 0), ("gather", 1)]
    steps += [("last", 0), ("last", 1), ("mix", 0)]
    steps += [("gather", m) for m in order[2:-1]]
    return steps + [("mix_contract", 0), ("gather", order[-1])]


def experts_kernel(
    n_ep,
    mix_hbm,
    mix_gain_hbm,
    kernel_hbm,
    group_gain_hbm,
    x_hbm,
    gain_hbm,
    routes_hbm,
    weight_hbm,
    outer_hbm,
    inner_hbm,
    value_hbm,
    mix_out_hbm,
    gate_hbm,
    up_hbm,
    down_hbm,
    mix_o_ref,
    o_ref,
    mix_ref,
    mix_gain_ref,
    kernel_ref,
    group_gain_ref,
    x_ref,
    gain_ref,
    routes_ref,
    weight_ref,
    nb,
    xs,
    xb,
    wgu,
    wd,
    hb,
    rs,
    ret,
    whi,
    wlo,
    total,
    na,
    wmix,
    wmo,
    padded,
    outer,
    grouped,
    i_sem,
    w_sem,
    s_sem,
    r_sem,
):
    ep = lax.axis_index("ep")
    tp = lax.axis_index("tp")
    y, core = tp // 2, tp % 2
    partner = {"tp": y * 2 + 1 - core}
    across = {"tp": (1 - y) * 2 + core}
    over_tp = (1 - y) * 2 + core
    half = n_ep // 2
    quarter = half // 2
    inner = (ep // half + ep // quarter) % 2
    rows = x_ref.shape[0]
    cap = xb.shape[2]
    span = xb.shape[3]
    tiles, depth, pair = wgu.shape
    tile = pair // 2
    part = hb.shape[3]
    out_cols = wd.shape[1]

    barrier = pltpu.get_barrier_semaphore()
    peers = [{"ep": flip(ep, m, n_ep)} for m in range(1, n_ep)] + [partner, across]

    chunk = 64
    chunks = rows // chunk
    fetch_x = [
        pltpu.make_async_copy(
            x_hbm.at[pl.ds(i * chunk, chunk)], x_ref.at[pl.ds(i * chunk, chunk)], i_sem.at[i]
        )
        for i in range(chunks)
    ]
    fetch_small = [
        pltpu.make_async_copy(src, dst, i_sem.at[chunks + i])
        for i, (src, dst) in enumerate(
            (
                (gain_hbm, gain_ref),
                (routes_hbm, routes_ref),
                (weight_hbm, weight_ref),
                (mix_gain_hbm, mix_gain_ref),
                (kernel_hbm, kernel_ref),
                (group_gain_hbm, group_gain_ref),
                (mix_hbm, mix_ref),
            )
        )
    ]
    fetches = []
    for j in range(tiles):
        cols = pl.ds(j * tile, tile)
        fetches.append(
            (
                pltpu.make_async_copy(
                    gate_hbm.at[0, :, cols], wgu.at[j, :, pl.ds(0, tile)], w_sem.at[2 * j]
                ),
                pltpu.make_async_copy(
                    up_hbm.at[0, :, cols], wgu.at[j, :, pl.ds(tile, tile)], w_sem.at[2 * j + 1]
                ),
            )
        )
    fetch_down = pltpu.make_async_copy(down_hbm.at[0], wd, w_sem.at[2 * tiles])
    fetch_mix = [
        pltpu.make_async_copy(src, wmix.at[i], w_sem.at[2 * tiles + 1 + i])
        for i, src in enumerate((outer_hbm, inner_hbm, value_hbm))
    ]
    fetch_mix_out = pltpu.make_async_copy(mix_out_hbm, wmo, w_sem.at[2 * tiles + 4])
    for copy in fetch_x:
        copy.start()
    for copy in fetch_small[:-1]:
        copy.start()
    for peer in peers:
        pl.semaphore_signal(barrier, inc=1, device_id=peer, device_id_type=pl.DeviceIdType.MESH)
    for a, b in fetches:
        a.start()
        b.start()

    step_rows = 32

    def normalize(src, gain, dst, start, count):
        def norm(i, carry):
            at = pl.ds(pl.multiple_of(i * step_rows, step_rows), step_rows)
            v = src[at, :].astype(F32)
            scale = lax.rsqrt(jnp.mean(v * v, axis=-1, keepdims=True) + EPS)
            dst[at, :] = (v * scale * gain[...]).astype(BF16)
            return carry

        lax.fori_loop(start // step_rows, (start + count) // step_rows, norm, 0)

    fetch_small[0].wait()
    for i in range(chunks):
        fetch_x[i].wait()
        normalize(x_ref, gain_ref, nb, i * chunk, chunk)
    fetch_small[-1].start()
    for copy in fetch_mix:
        copy.start()
    fetch_down.start()
    fetch_mix_out.start()

    fetch_small[1].wait()
    first = routes_ref[0:1, :]
    second = routes_ref[1:2, :]
    masks = []
    level = lax.broadcasted_iota(jnp.int32, (n_ep, rows), 0)
    stacked = jnp.zeros((n_ep, rows), F32)
    for m in range(n_ep):
        e = flip(ep, m, n_ep)
        mask = jnp.where((first == e) | (second == e), 1.0, 0.0)
        masks.append(mask)
        stacked = jnp.where(level == m, mask, stacked)
    upper = lax.broadcasted_iota(jnp.int32, (rows, rows), 0) < lax.broadcasted_iota(
        jnp.int32, (rows, rows), 1
    )
    ranks = matmul(stacked.astype(BF16), jnp.where(upper, 1.0, 0.0).astype(BF16))
    slots = lax.broadcasted_iota(jnp.int32, (cap, rows), 0).astype(F32)

    def place(m):
        return jnp.where((slots == ranks[m : m + 1, :]) & (masks[m] > 0.5), 1.0, 0.0)

    def remote(src, dst, kind, m, device):
        return pltpu.make_async_remote_copy(
            src_ref=src,
            dst_ref=dst,
            send_sem=s_sem.at[kind, m],
            recv_sem=r_sem.at[kind, m],
            device_id=device,
            device_id_type=pl.DeviceIdType.MESH,
        )

    def label(turn):
        if turn < half:
            return turn
        r = turn - half
        return turn + (1 - inner) * (quarter - 2 * quarter * (r // quarter))

    def source_of(m):
        return {"ep": flip(ep, m, n_ep)}

    mine2 = pl.ds(core * 2, 2)

    def near_rows(m):
        return remote(xs.at[m], xb.at[m, mine2], 0, m, source_of(m))

    def near_partner(m):
        return remote(xb.at[m, mine2], xb.at[m, mine2], 1, m, partner)

    def far_rows(m):
        return remote(xs.at[m, 0], xb.at[m, tp], 0, m, source_of(m))

    def far_rows_over(m):
        return remote(xs.at[m, 1], xb.at[m, over_tp], 12, m, source_of(m))

    def far_partner(m):
        return remote(xb.at[m, tp], xb.at[m, tp], 1, m, partner)

    def far_across(m):
        return remote(xb.at[m, tp], xb.at[m, tp], 2, m, across)

    def far_relay(m):
        return remote(xb.at[m, over_tp], xb.at[m, over_tp], 3, m, partner)

    mid = (tiles + 1) // 2
    pieces = [(0, mid), (mid, tiles)]

    final = turns(n_ep)[-1]
    half_cap = cap // 2

    def final_turn(m):
        return isinstance(m, int) and m == final

    def hidden_piece(m, where, p):
        if final_turn(m):
            return hb.at[m, where, pl.ds(p * half_cap, half_cap)]
        lo, hi = pieces[p]
        return hb.at[m, where, :, pl.ds(lo * tile, (hi - lo) * tile)]

    def hid_partner(m, p):
        return remote(hidden_piece(m, tp, p), hidden_piece(m, tp, p), 4 + 5 * p, m, partner)

    def hid_across(m, p):
        return remote(hidden_piece(m, tp, p), hidden_piece(m, tp, p), 5 + 5 * p, m, across)

    def hid_relay(m, p):
        return remote(hidden_piece(m, over_tp, p), hidden_piece(m, over_tp, p), 6 + 5 * p, m, partner)

    def back(m):
        return remote(rs.at[m], ret.at[m], 7, m, source_of(m))

    def back_final(p):
        at = pl.ds(p * half_cap, half_cap)
        return remote(rs.at[final, at], ret.at[final, at], 7 + 6 * p, final, source_of(final))

    def dispatch(m):
        chosen = place(m).astype(BF16)
        if m < half:
            for k in range(2):
                at = pl.ds(pl.multiple_of((core * 2 + k) * span, span), span)
                xs[m, k] = matmul(chosen, nb[:, at]).astype(BF16)
        else:
            at = pl.ds(pl.multiple_of(tp * span, span), span)
            xs[m, 0] = matmul(chosen, nb[:, at]).astype(BF16)
            if m % quarter + half + quarter in doubled(n_ep):
                at = pl.ds(pl.multiple_of(over_tp * span, span), span)
                xs[m, 1] = matmul(chosen, nb[:, at]).astype(BF16)
        if m == 1:
            pl.semaphore_wait(barrier, len(peers))
        if m < half:
            near_rows(m).start()
        else:
            far_rows(m).start()
            if m % quarter + half + quarter in doubled(n_ep):

                @pl.when(inner == 1)
                def _():
                    far_rows_over(m).start()

    def expand(turn):
        m = label(turn)

        def body(j, carry):
            if turn == 0:
                pltpu.make_async_copy(
                    gate_hbm.at[0, :, pl.ds(0, tile)], wgu.at[j, :, pl.ds(0, tile)], w_sem.at[2 * j]
                ).wait()
                pltpu.make_async_copy(
                    up_hbm.at[0, :, pl.ds(0, tile)],
                    wgu.at[j, :, pl.ds(tile, tile)],
                    w_sem.at[2 * j + 1],
                ).wait()
            acc = matmul(xb[m, 0], wgu[j, 0:span, :])
            for k in range(1, depth // span):
                acc = acc + matmul(xb[m, k], wgu[j, k * span : (k + 1) * span, :])
            g, u = acc[:, :tile], acc[:, tile:]
            hidden = g / (1.0 + jnp.exp(-g)) * u
            hb[m, tp, :, pl.ds(pl.multiple_of(j * tile, tile), tile)] = hidden.astype(BF16)
            return carry

        for p, (lo, hi) in enumerate(pieces):
            lax.fori_loop(lo, hi, body, 0)
            if not final_turn(m):
                hid_across(m, p).start()
                hid_partner(m, p).start()
        if final_turn(m):
            for p in range(2):
                hid_across(m, p).start()
                hid_partner(m, p).start()

    block = 256

    def contract(turn):
        m = label(turn)
        for p in range(len(pieces)):
            hid_partner(m, p).wait_recv()
            hid_relay(m, p).wait_recv()
        for n in range(out_cols // block):
            cols = slice(n * block, (n + 1) * block)
            acc = matmul(hb[m, 0], wd[0:part, cols])
            for k in range(1, hb.shape[1]):
                acc = acc + matmul(hb[m, k], wd[k * part : (k + 1) * part, cols])
            if turn == 0:
                ret[0, :, cols] = acc.astype(BF16)
            else:
                rs[m, :, cols] = acc.astype(BF16)
        if turn:
            back(m).start()

    def last(p):
        if p == 0:
            hid_across(final, 0).wait_recv()
            hid_relay(final, 0).start()
        hid_partner(final, p).wait_recv()
        hid_relay(final, p).wait_recv()
        at = slice(p * half_cap, (p + 1) * half_cap)
        for n in range(out_cols // block):
            cols = slice(n * block, (n + 1) * block)
            acc = matmul(hb[final, 0, at], wd[0:part, cols])
            for k in range(1, hb.shape[1]):
                acc = acc + matmul(hb[final, k, at], wd[k * part : (k + 1) * part, cols])
            rs[final, at, cols] = acc.astype(BF16)
        back_final(p).start()
        if p == 0:
            hid_across(final, 1).wait_recv()
            hid_relay(final, 1).start()

    def pass_hidden(turn):
        for p in range(len(pieces)):
            hid_across(label(turn), p).wait_recv()
            hid_relay(label(turn), p).start()

    def pass_near(m):
        near_rows(m).wait_recv()
        near_partner(m).start()

    def pass_both(turn):
        m = label(turn)
        far_rows(m).wait_recv()
        far_partner(m).start()
        far_rows_over(m).wait_recv()
        far_relay(m).start()

    def pass_far(turn):
        m = label(turn)
        far_rows(m).wait_recv()
        far_across(m).start()
        far_partner(m).start()

    def pass_relay(turn):
        m = label(turn)
        far_across(m).wait_recv()
        far_relay(m).start()

    def ready(turn):
        m = label(turn)
        if turn < half:
            near_partner(m).wait_recv()
        else:
            far_partner(m).wait_recv()
            far_relay(m).wait_recv()

    mix_rows, channels = outer.shape
    halo = padded.shape[0] - mix_rows
    ahead = {"ep": lax.rem(ep + 1, n_ep)}
    send_halo = remote(padded.at[pl.ds(mix_rows, halo)], padded.at[pl.ds(0, halo)], 8, 0, ahead)
    mix_partner = remote(grouped.at[tp], grouped.at[tp], 8, 1, partner)
    mix_across = remote(grouped.at[tp], grouped.at[tp], 8, 2, across)
    mix_relay = remote(grouped.at[over_tp], grouped.at[over_tp], 8, 3, partner)

    def mix_project():
        for copy in fetch_small[3:]:
            copy.wait()
        normalize(mix_ref, mix_gain_ref, na, 0, mix_rows)
        for copy in fetch_mix:
            copy.wait()
        outer[...] = matmul(na[...], wmix[0]).astype(BF16)
        inner = matmul(na[...], wmix[1]).astype(BF16).astype(F32)
        padded[pl.ds(halo, mix_rows), :] = inner * matmul(na[...], wmix[2]).astype(BF16).astype(F32)

        @pl.when(ep < n_ep - 1)
        def _():
            send_halo.start()

        @pl.when(ep == 0)
        def _():
            padded[pl.ds(0, halo), :] = jnp.zeros((halo, channels), F32)

    def mix_convolve(_):
        @pl.when(ep > 0)
        def _():
            send_halo.wait_recv()

        taps = kernel_ref[...].astype(F32)
        conv = taps[2:3, :] * padded[pl.ds(halo, mix_rows), :]
        for back_by in (1, 2):
            conv = conv + taps[2 - back_by : 3 - back_by, :] * padded[pl.ds(halo - back_by, mix_rows), :]
        gated = outer[...].astype(F32) * conv
        squares = gated * gated
        group = lax.broadcasted_iota(jnp.int32, (mix_rows, channels), 1) // GROUP
        scale = jnp.zeros_like(gated)
        for i in range(channels // GROUP):
            mean = jnp.sum(jnp.where(group == i, squares, 0.0), axis=-1, keepdims=True) / GROUP
            scale = jnp.where(group == i, lax.rsqrt(mean + EPS), scale)
        grouped[tp] = (gated * scale * group_gain_ref[...]).astype(BF16)
        mix_across.start()
        mix_partner.start()

    def mix_pass(_):
        mix_across.wait_recv()
        mix_relay.start()

    def mix_contract(_):
        fetch_mix_out.wait()
        mix_partner.wait_recv()
        mix_relay.wait_recv()
        acc = matmul(grouped[0], wmo[0:channels, :])
        for k in range(1, grouped.shape[0]):
            acc = acc + matmul(grouped[k], wmo[k * channels : (k + 1) * channels, :])
        mix_o_ref[...] = acc.astype(BF16)

    def build_weights():
        fetch_small[2].wait()
        for m in range(n_ep):
            picked = jnp.where(first == flip(ep, m, n_ep), weight_ref[0:1, :], weight_ref[1:2, :])
            scaled = (place(m) * picked).T
            high = scaled.astype(BF16)
            whi[:, m * cap : (m + 1) * cap] = high
            wlo[:, m * cap : (m + 1) * cap] = (scaled - high.astype(F32)).astype(BF16)

    def gather(turn):
        m = label(turn)
        if turn == final:
            back_final(0).wait_recv()
            back_final(1).wait_recv()
        elif turn:
            back(m).wait_recv()
        cols = pl.ds(m * cap if turn < half else pl.multiple_of(m * cap, cap), cap)
        high = matmul(whi[:, cols], ret[m])
        low = matmul(wlo[:, cols], ret[m])
        if turn == 0:
            total[...] = high + low
        else:
            total[...] += high + low

    first_sends, later_sends, last_sends = send_order(n_ep)
    for m in first_sends:
        dispatch(m)
    chosen = place(0).astype(BF16)
    for k in range(depth // span):
        xb[0, k] = matmul(chosen, nb[:, k * span : (k + 1) * span]).astype(BF16)
    expand(0)
    for m in later_sends:
        dispatch(m)
    mix_project()
    build_weights()
    for m in last_sends:
        dispatch(m)
    fetch_down.wait()
    actions = dict(
        last=last, near=pass_near, both=pass_both, pass_far=pass_far, far=pass_relay, ready=ready, expand=expand,
        hidden=pass_hidden, contract=contract, mix_convolve=mix_convolve, mix=mix_pass,
        gather=gather, mix_contract=mix_contract,
    )
    for step, m in schedule(n_ep):
        actions[step](m)
    o_ref[...] = total[...].astype(BF16)

    @pl.when(ep < n_ep - 1)
    def _():
        send_halo.wait_send()

    for copy in (mix_partner, mix_across, mix_relay):
        copy.wait_send()
    for turn in range(n_ep):
        m = label(turn)
        for p in range(len(pieces)):
            for copy in (hid_partner(m, p), hid_across(m, p), hid_relay(m, p)):
                copy.wait_send()
        if turn == final:
            back_final(0).wait_send()
            back_final(1).wait_send()
        elif turn:
            back(m).wait_send()
        if 0 < turn < half:
            near_rows(m).wait_send()
            near_partner(m).wait_send()
        if turn >= half:
            far_rows(m).wait_send()
            far_partner(m).wait_send()
            far_relay(m).wait_send()
            if turn not in doubled(n_ep):
                far_across(m).wait_send()
            if turn % quarter + half + quarter in doubled(n_ep):

                @pl.when(inner == 1)
                def _():
                    far_rows_over(m).wait_send()


def fused(
    mixer_input,
    mixer_gain,
    outer_weight,
    inner_weight,
    value_weight,
    conv_kernel,
    group_gain,
    mixer_out_weight,
    expert_input,
    expert_gain,
    routes,
    route_weight,
    expert_gate,
    expert_up,
    expert_down,
):
    n_ep, n_tp = lax.axis_size("ep"), lax.axis_size("tp")
    rows, width = expert_input.shape
    mix_rows = mixer_input.shape[0]
    channels = outer_weight.shape[1]
    cap = 2 * routes.shape[1] * rows // n_ep
    span = width // n_tp
    part = expert_gate.shape[2]
    tile = 128
    tiles = part // tile
    full, out_cols = expert_down.shape[1:]
    mix_cols = mixer_out_weight.shape[1]
    vmem = pl.BlockSpec(memory_space=pltpu.VMEM)
    hbm = pl.BlockSpec(memory_space=pl.ANY)
    operands = (
        mixer_input,
        mixer_gain.reshape(1, -1),
        conv_kernel,
        group_gain.reshape(1, -1),
        expert_input,
        expert_gain.reshape(1, -1),
        routes.T,
        route_weight.T,
        outer_weight,
        inner_weight,
        value_weight,
        mixer_out_weight,
        expert_gate,
        expert_up,
        expert_down,
    )
    return pl.pallas_call(
        functools.partial(experts_kernel, n_ep),
        out_shape=(
            pltpu.VMEM((mix_rows, mix_cols), BF16),
            pltpu.VMEM((rows, out_cols), BF16),
        ),
        in_specs=[hbm] * len(operands),
        out_specs=(vmem, vmem),
        scratch_shapes=[
            *(pltpu.VMEM(v.shape, v.dtype) for v in operands[:8]),
            pltpu.VMEM((rows, width), BF16),
            pltpu.VMEM((n_ep, 2, cap, span), BF16),
            pltpu.VMEM((n_ep, n_tp, cap, span), BF16),
            pltpu.VMEM((tiles, width, 2 * tile), BF16),
            pltpu.VMEM((full, out_cols), BF16),
            pltpu.VMEM((n_ep, n_tp, cap, part), BF16),
            pltpu.VMEM((n_ep, cap, out_cols), BF16),
            pltpu.VMEM((n_ep, cap, out_cols), BF16),
            pltpu.VMEM((rows, n_ep * cap), BF16),
            pltpu.VMEM((rows, n_ep * cap), BF16),
            pltpu.VMEM((rows, out_cols), F32),
            pltpu.VMEM((mix_rows, width), BF16),
            pltpu.VMEM((3, width, channels), BF16),
            pltpu.VMEM((channels * n_tp, mix_cols), BF16),
            pltpu.VMEM((8 + mix_rows, channels), F32),
            pltpu.VMEM((mix_rows, channels), BF16),
            pltpu.VMEM((n_tp, mix_rows, channels), BF16),
            pltpu.SemaphoreType.DMA((rows // 64 + 7,)),
            pltpu.SemaphoreType.DMA((2 * tiles + 5,)),
            pltpu.SemaphoreType.DMA((14, n_ep)),
            pltpu.SemaphoreType.DMA((14, n_ep)),
        ],
        compiler_params=pltpu.CompilerParams(
            collective_id=0, has_side_effects=True, vmem_limit_bytes=60 * 1024 * 1024
        ),
        name="layer",
    )(*operands)


def fits(n_ep, n_tp, routes, expert_gate):
    return (
        n_tp == 4
        and n_ep >= 8
        and n_ep & (n_ep - 1) == 0
        and routes.shape[1] == 2
        and expert_gate.shape[0] == 1
        and expert_gate.shape[2] % 128 == 0
        and routes.shape[0] % 64 == 0
    )


def mixer_xla(
    mixer_input,
    mixer_gain,
    outer_weight,
    inner_weight,
    value_weight,
    conv_kernel,
    group_gain,
    mixer_out_weight,
):
    mix_count = mixer_input.shape[0]
    normed_a = rms_scale(mixer_input, mixer_gain).astype(jnp.bfloat16)
    outer = jnp.dot(normed_a, outer_weight, preferred_element_type=jnp.float32).astype(jnp.bfloat16)
    inner = jnp.dot(normed_a, inner_weight, preferred_element_type=jnp.float32).astype(jnp.bfloat16)
    values = jnp.dot(normed_a, value_weight, preferred_element_type=jnp.float32).astype(
        jnp.bfloat16
    )
    product = inner.astype(jnp.float32) * values.astype(jnp.float32)
    earlier_rows = from_behind(product[mix_count - 2 :], "ep", 1)
    padded = jnp.concatenate([earlier_rows, product], axis=0)
    kernel = conv_kernel.astype(jnp.float32)
    conv_sum = (
        kernel[0] * padded[0:mix_count]
        + kernel[1] * padded[1 : mix_count + 1]
        + kernel[2] * padded[2 : mix_count + 2]
    )
    gated = outer.astype(jnp.float32) * conv_sum
    grouped = gated.reshape(mix_count, -1, GROUP)
    grouped = rms_scale(grouped, group_gain.reshape(-1, GROUP))
    grouped = grouped.reshape(mix_count, -1).astype(jnp.bfloat16)
    weight_rows = mixer_out_weight
    mixed_tokens = jnp.dot(
        lax.all_gather(grouped, "tp", axis=1, tiled=True),
        weight_rows,
        preferred_element_type=jnp.float32,
    ).astype(jnp.bfloat16)
    return mixed_tokens


def experts_xla(
    expert_input,
    expert_gain,
    routes,
    route_weight,
    expert_gate,
    expert_up,
    expert_down,
):
    exp_count, picks_each = routes.shape
    width = expert_input.shape[1]
    experts = expert_gate.shape[0] * lax.axis_size("ep")
    capacity = 2 * picks_each * exp_count // experts
    normed_b = rms_scale(expert_input, expert_gain).astype(jnp.bfloat16)
    picks = routes.reshape(-1)
    onehot = (picks[:, None] == jnp.arange(experts, dtype=jnp.int32)[None, :]).astype(jnp.int32)
    rank = jnp.sum((jnp.cumsum(onehot, axis=0) - onehot) * onehot, axis=1)
    slot = picks * capacity + rank
    token = jnp.arange(exp_count * picks_each, dtype=jnp.int32) // picks_each
    table = jnp.zeros((experts * capacity,), jnp.int32).at[slot].set(token + 1)
    valid = table > 0
    gathered_rows = jnp.take(normed_b, jnp.maximum(table - 1, 0), axis=0)
    buffer = jnp.where(valid[:, None], gathered_rows, 0).reshape(experts, capacity, width)
    gate_weight = expert_gate[0]
    up_weight = expert_up[0]
    down_weight = expert_down[0]
    out_cols = down_weight.shape[1]
    span = width // lax.axis_size("tp")
    outgoing = lax.dynamic_slice_in_dim(buffer, lax.axis_index("tp") * span, span, 2)
    received = lax.all_to_all(outgoing, "ep", split_axis=0, concat_axis=0, tiled=True)
    sources = received.shape[0]
    count = received.shape[1]
    piece = lax.all_gather(received, "tp", axis=2, tiled=True)
    span = piece.shape[2]
    flat_piece = piece.reshape(sources * count, span)
    gate = jnp.dot(flat_piece, gate_weight, preferred_element_type=jnp.float32)
    up_value = jnp.dot(flat_piece, up_weight, preferred_element_type=jnp.float32)
    hidden = (jax.nn.silu(gate) * up_value).astype(jnp.bfloat16)
    weight_rows = down_weight
    results = jnp.dot(
        lax.all_gather(hidden, "tp", axis=1, tiled=True),
        weight_rows,
        preferred_element_type=jnp.float32,
    ).astype(jnp.bfloat16)
    returned = lax.all_to_all(
        results.reshape(sources, count, out_cols), "ep", split_axis=0, concat_axis=0, tiled=True
    )
    flat_returned = returned.reshape(experts * capacity, out_cols)
    chosen = (
        jnp.take(flat_returned, slot, axis=0)
        .astype(jnp.float32)
        .reshape(exp_count, picks_each, out_cols)
    )
    weighted = jnp.sum(chosen * route_weight[..., None], axis=1)
    expert_tokens = weighted.astype(jnp.bfloat16)
    return expert_tokens


def per_device(*args):
    n_ep, n_tp = lax.axis_size("ep"), lax.axis_size("tp")
    if fits(n_ep, n_tp, args[10], args[12]):
        return fused(*args)
    return mixer_xla(*args[:8]), experts_xla(*args[8:])


def solution(mesh):
    placed = (
        P("ep", None),
        P(),
        P(None, "tp"),
        P(None, "tp"),
        P(None, "tp"),
        P(None, "tp"),
        P("tp"),
        P(None, "tp"),
        P("ep", None),
        P(),
        P("ep", None),
        P("ep", None),
        P("ep", None, "tp"),
        P("ep", None, "tp"),
        P("ep", None, "tp"),
    )
    return jax.shard_map(
        per_device,
        mesh=mesh,
        in_specs=placed,
        out_specs=(P("ep", "tp"), P("ep", "tp")),
        check_vma=False,
    )
```
